512 devices in a mesh: sp: 128 (over z, y, core), tp: 4 (over x).
Axes of the slice: x: 4, y: 8, z: 8, core: 2. Of those that a mesh axis runs over, the one named last changes fastest.
Arguments:
- tokens: bfloat16 [32768, 2048], P(('sp', 'tp')), may hold values from -16 to 16
- w_query: bfloat16 [2048, 1024], P(None, 'tp'), may hold values from -1 to 1
- w_key: bfloat16 [2048, 256], P(None, 'tp'), may hold values from -1 to 1
- w_value: bfloat16 [2048, 256], P(None, 'tp'), may hold values from -0.125 to 0.125
- w_gate: bfloat16 [2048, 16], P(None, 'tp'), may hold values from -0.125 to 0.125
- gate_bias: float32 [16], P('tp'), as said below
- w_output: bfloat16 [1024, 2048], P('tp'), may hold values from -0.1875 to 0.1875
Outputs:
- mixed: bfloat16 [32768, 2048], P(('sp', 'tp'))
The draws below stay inside these ranges and needn't reach their ends.
Inputs may be any that keep to these rules, and one draw needn't show every extreme that they name: `gate_bias`: each head's forget gate bias is 4 or more; there is no upper bound.
All inputs are finite; a program needn't handle non-finite values.
Results may differ from the reference program's by a relative error of at most 0.012.
The reference program's roundings to bfloat16 on the way count: a program that leaves them out, or rounds other values in their place, can miss the bound.
Values may be sent and summed in bfloat16 or wider, within the bound.
A program may use at most 64 MiB of HBM per device.

```python
import math
import jax
import jax.numpy as jnp
from jax import lax

D = 2048
HEADS = 16
KV_HEADS = 4
HEAD = 64
TOK_DEV = 256
SEQ = 32768
N_TP = 4


def query_base(base_key):
    raw_values = jax.random.normal(jax.random.fold_in(base_key, 11), (D, HEADS * HEAD), jnp.float32)
    return jnp.clip(raw_values, -5.0, 5.0) / math.sqrt(D)


def draw_w_query(key, part):
    return query_base(key).astype(jnp.bfloat16)


def draw_w_key(key, part):
    raw_values = jax.random.normal(jax.random.fold_in(key, 12), (D, KV_HEADS * HEAD), jnp.float32)
    return (jnp.clip(raw_values, -5.0, 5.0) / math.sqrt(D)).astype(jnp.bfloat16)


def draw_gate_bias(key, part):
    shuffled = jax.random.permutation(jax.random.fold_in(key, 21), HEADS)
    quick = shuffled < HEADS // 2
    lasting = math.log(SEQ) + jax.random.uniform(jax.random.fold_in(key, 22), (HEADS,), jnp.float32, 0.5, 1.5)
    fading = jax.random.uniform(jax.random.fold_in(key, 23), (HEADS,), jnp.float32, 4.1, 5.3)
    return jnp.where(quick, fading, lasting).astype(jnp.float32)


def draw_tokens(key, part):
    span_rows = TOK_DEV // 2
    span_count = SEQ // span_rows
    scales = jnp.exp(jax.random.uniform(jax.random.fold_in(key, 31), (span_count, 1, 1), jnp.float32, math.log(0.6), math.log(1.6)))
    shifts = jax.random.uniform(jax.random.fold_in(key, 32), (span_count, 1, 1), jnp.float32, -1.5, 1.5)
    heading = jnp.clip(jax.random.normal(jax.random.fold_in(key, 33), (1, 1, D), jnp.float32), -3.0, 3.0)
    noise = jnp.clip(jax.random.normal(jax.random.fold_in(key, 34), (span_count, span_rows, D), jnp.float32), -5.0, 5.0)
    field = (scales * (noise + shifts * heading)).reshape(SEQ, D)
    return jnp.clip(field, -16.0, 16.0).astype(jnp.bfloat16)


def block_levels(stream_key, dims, pieces, low, largest):
    loudness = 1.0
    for axis_at, shards_of in pieces:
        steps = jax.random.uniform(jax.random.fold_in(jax.random.fold_in(stream_key, 6), axis_at), (shards_of,), jnp.float32, low / len(pieces), largest / len(pieces))
        loudness = loudness * jnp.repeat(jnp.exp(steps), dims[axis_at] // shards_of).reshape((-1,) + (1,) * (len(dims) - 1 - axis_at))
    return loudness


def normal_values(key, extent, deviation, reach, shards=(), kind=jnp.bfloat16):
    values = jax.random.normal(key, extent, jnp.float32) * deviation
    if len(shards) > 0:
        values = block_levels(key, extent, shards, -0.22, 0.18) * values
    return jnp.clip(values, min=-reach, max=reach).astype(kind)


def setup_inputs(seed: int = 0) -> dict:
    splits = jax.random.split(jax.random.key(seed), 8)
    return {
        "tokens": draw_tokens(jax.random.fold_in(splits[7], 71), 0),
        "w_query": draw_w_query(jax.random.fold_in(splits[7], 71), 0),
        "w_key": draw_w_key(jax.random.fold_in(splits[7], 71), 0),
        "w_value": normal_values(splits[3], (D, KV_HEADS * HEAD), D ** -0.5, 0.125, ((1, 4),)),
        "w_gate": normal_values(splits[4], (D, HEADS), D ** -0.5, 0.125, ((1, 4),)),
        "gate_bias": draw_gate_bias(jax.random.fold_in(splits[7], 71), 0),
        "w_output": normal_values(splits[6], (HEADS * HEAD, D), (HEADS * HEAD) ** -0.5, 0.1875, ((0, 4),)),
    }


masked_value = -1e30


def reference(tokens, w_query, w_key, w_value, w_gate, gate_bias, w_output):
    length = tokens.shape[0]
    group_size = HEADS // KV_HEADS
    queries = jnp.dot(tokens, w_query, preferred_element_type=jnp.float32).astype(jnp.bfloat16)
    key_proj = jnp.dot(tokens, w_key, preferred_element_type=jnp.float32).astype(jnp.bfloat16)
    value_proj = jnp.dot(tokens, w_value, preferred_element_type=jnp.float32).astype(jnp.bfloat16)
    gate_logits = jnp.dot(tokens, w_gate, preferred_element_type=jnp.float32).astype(jnp.bfloat16)
    queries, key_proj, value_proj, gate_logits = lax.optimization_barrier((queries, key_proj, value_proj, gate_logits))
    log_gates = jax.nn.log_sigmoid(gate_logits.astype(jnp.float32) + gate_bias.astype(jnp.float32))
    cumulative = jnp.cumsum(log_gates, axis=0)
    span = math.gcd(length, 512)
    block_total = length // span
    query_all = queries.astype(jnp.float32).reshape(block_total, span, KV_HEADS, group_size, HEAD)
    key_all = key_proj.astype(jnp.float32).reshape(block_total, span, KV_HEADS, HEAD)
    value_all = value_proj.astype(jnp.float32).reshape(block_total, span, KV_HEADS, HEAD)
    cumul_all = cumulative.reshape(block_total, span, KV_HEADS, group_size)
    scale = HEAD ** -0.5

    def query_block(block_index):
        query_here = lax.dynamic_index_in_dim(query_all, block_index, 0, keepdims=False)
        cumul_here = lax.dynamic_index_in_dim(cumul_all, block_index, 0, keepdims=False).transpose(1, 2, 0)
        query_position = block_index * span + jnp.arange(span, dtype=jnp.int32)

        def key_step(key_index, carry_state):
            row_peak, row_mass, row_accum = carry_state
            key_here = lax.dynamic_index_in_dim(key_all, key_index, 0, keepdims=False)
            value_here = lax.dynamic_index_in_dim(value_all, key_index, 0, keepdims=False)
            key_cumul = lax.dynamic_index_in_dim(cumul_all, key_index, 0, keepdims=False).transpose(1, 2, 0)
            key_position = key_index * span + jnp.arange(span, dtype=jnp.int32)
            scores = jnp.einsum("tkgd,skd->kgts", query_here, key_here) * scale
            scores = scores + cumul_here[:, :, :, None] - key_cumul[:, :, None, :]
            allowed = key_position[None, :] <= query_position[:, None]
            scores = jnp.where(allowed, scores, masked_value)
            new_peak = jnp.maximum(row_peak, jnp.max(scores, axis=3))
            weights = jnp.where(allowed, jnp.exp(scores - new_peak[:, :, :, None]), 0.0)
            rescale = jnp.exp(row_peak - new_peak)
            row_mass = row_mass * rescale + jnp.sum(weights, axis=3)
            weights_low = lax.optimization_barrier(weights.astype(jnp.bfloat16))
            row_accum = row_accum * rescale[:, :, :, None] + jnp.einsum(
                "kgts,skd->kgtd", weights_low.astype(jnp.float32), value_here)
            return new_peak, row_mass, row_accum

        initial = (jnp.full((KV_HEADS, group_size, span), masked_value, jnp.float32),
                   jnp.zeros((KV_HEADS, group_size, span), jnp.float32),
                   jnp.zeros((KV_HEADS, group_size, span, HEAD), jnp.float32))
        row_peak, row_mass, row_accum = lax.fori_loop(0, block_index + 1, key_step, initial)
        attended = (row_accum / row_mass[:, :, :, None]).astype(jnp.bfloat16)
        return attended.transpose(2, 0, 1, 3).reshape(span, HEADS * HEAD)

    attended = lax.map(query_block, jnp.arange(block_total, dtype=jnp.int32)).reshape(length, HEADS * HEAD)
    per_group = HEADS * HEAD // N_TP
    total = jnp.zeros((length, D), jnp.float32)
    for group_index in range(N_TP):
        partial_value = jnp.dot(attended[:, group_index * per_group:(group_index + 1) * per_group],
                          w_output[group_index * per_group:(group_index + 1) * per_group],
                          preferred_element_type=jnp.float32).astype(jnp.bfloat16)
        partial_value = lax.optimization_barrier(partial_value)
        total = total + partial_value.astype(jnp.float32)
    return total.astype(jnp.bfloat16)
```

```python
import functools

import jax
import jax.numpy as jnp
from jax import lax
from jax.experimental import pallas as pl
from jax.experimental.pallas import tpu as pltpu
from jax.sharding import Mesh
from jax.sharding import PartitionSpec as P

HEAD = 64
BLOCK = 256
HALF = 128
ROWS = 144
LOG2E = 1.4426950408889634
LOW = -1e30
AXES = ("sp_0", "sp_1", "sp_2", "tp")
SP_TP = AXES
MESH = pl.DeviceIdType.MESH
f32 = jnp.float32
bf16 = jnp.bfloat16


def place():
    return tuple(lax.axis_index(a) for a in AXES)


def greet(peers):
    barrier = pltpu.get_barrier_semaphore()
    for peer in peers:
        pl.semaphore_signal(barrier, inc=1, device_id=peer, device_id_type=MESH)
    pl.semaphore_wait(barrier, len(peers))


def remote(src, dst, send, recv, device):
    return pltpu.make_async_remote_copy(
        src_ref=src, dst_ref=dst, send_sem=send, recv_sem=recv,
        device_id=device, device_id_type=MESH,
    )


def three(x):
    a = x.astype(bf16).astype(f32)
    r = x - a
    b = r.astype(bf16).astype(f32)
    return a, b, r - b


def iota(shape, dim):
    return lax.broadcasted_iota(jnp.int32, shape, dim)


def project_kernel(
    tokens, w_q, w_k, w_v, w_g, bias, kv_out, q_out,
    x_all, wq_v, wk_v, wv_v, wg_v, send, recv, local,
):
    z, y, c, x = place()
    n = 4
    peers = [(z, y, c, lax.rem(x + k, n)) for k in range(1, n)]
    loads = [
        pltpu.make_async_copy(src, dst, local.at[i])
        for i, (src, dst) in enumerate(((w_q, wq_v), (w_k, wk_v), (w_v, wv_v), (w_g, wg_v)))
    ]
    for load in loads:
        load.start()
    greet(peers)
    copies = [
        remote(tokens, x_all.at[x], send.at[k], recv.at[k], peers[k]) for k in (0, 2, 1)
    ]
    for copy in copies:
        copy.start()
    x_all[x] = tokens[...]
    for load in loads:
        load.wait()
    for copy in copies:
        copy.wait()
    rows = x_all[...].reshape(BLOCK, x_all.shape[2])

    def dot(a, b):
        return jnp.dot(a, b, preferred_element_type=f32)

    keys = dot(rows, wk_v[...]).astype(bf16).astype(f32)
    values = dot(rows, wv_v[...]).astype(bf16).astype(f32)
    kv = jnp.concatenate([keys, values], axis=1).T
    kv_out[0:HALF, :] = kv.astype(bf16)

    gates = dot(rows, wg_v[...]).astype(bf16).astype(f32) + bias[...]
    heads = gates.shape[1]
    gates = jnp.concatenate([gates, jnp.zeros((BLOCK, 128 - heads), f32)], axis=1).T[0:8]
    small = jnp.exp(-jnp.abs(gates))
    series = small * (1.0 - small * (0.5 - small * (1 / 3 - small * (0.25 - small * 0.2))))
    logs = jnp.minimum(gates, 0.0) - jnp.where(small < 0.02, series, jnp.log(1.0 + small))
    tri = (iota((BLOCK, BLOCK), 0) <= iota((BLOCK, BLOCK), 1)).astype(f32).astype(bf16)
    pieces = jnp.concatenate([*three(logs), jnp.zeros((8, BLOCK), f32)], axis=0)
    sums = dot(pieces.astype(bf16), tri)
    decay = (sums[0:8] + sums[8:16] + sums[16:24]) * (-LOG2E)
    hi, mid, lo = three(decay)
    row = iota((8, BLOCK), 0)
    first = jnp.where(row < 4, hi, pltpu.roll(mid, 4, 0))
    second = jnp.where(row < 4, lo, 0.0)
    kv_out[HALF:ROWS, :] = jnp.concatenate([first, second], axis=0).astype(bf16)

    queries = dot(rows, wq_v[...]).astype(bf16).astype(f32) * (LOG2E * HEAD**-0.5)
    top = queries.astype(bf16).astype(f32)
    rest = queries - top
    for h in range(4):
        cols = slice(h * HEAD, (h + 1) * HEAD)
        both = jnp.concatenate([top[:, cols], rest[:, cols]], axis=1).astype(bf16)
        for part in range(2):
            q_out[part, h * HALF : (h + 1) * HALF, :] = both[part * HALF : (part + 1) * HALF]


def project(tokens, w_q, w_k, w_v, w_g, bias):
    d = tokens.shape[1]
    vmem = pl.BlockSpec(memory_space=pltpu.VMEM)
    anyspace = pl.BlockSpec(memory_space=pl.ANY)
    return pl.pallas_call(
        project_kernel,
        name="project",
        out_shape=(
            jax.ShapeDtypeStruct((ROWS, BLOCK), bf16),
            jax.ShapeDtypeStruct((2, 4 * HALF, 128), bf16),
        ),
        in_specs=[vmem, anyspace, anyspace, anyspace, anyspace, vmem],
        out_specs=(vmem, vmem),
        scratch_shapes=[
            pltpu.VMEM((4, tokens.shape[0], d), bf16),
            pltpu.VMEM(w_q.shape, bf16),
            pltpu.VMEM(w_k.shape, bf16),
            pltpu.VMEM(w_v.shape, bf16),
            pltpu.VMEM(w_g.shape, bf16),
            pltpu.SemaphoreType.DMA((3,)),
            pltpu.SemaphoreType.DMA((3,)),
            pltpu.SemaphoreType.DMA((4,)),
        ],
        compiler_params=pltpu.CompilerParams(
            collective_id=0, has_side_effects=True, vmem_limit_bytes=24 * 2**20
        ),
    )(tokens, w_q, w_k, w_v, w_g, bias)


def block_rank(core, a, b):
    zz = a * (1 - core) + b * core
    yy = b * (1 - core) + a * core
    return zz * 16 + yy * 2 + core


def attend_kernel(
    own_kv, queries, w_own, att_out, w_all,
    buf, q_aug, q_in, peak, accum, table,
    local, one_send, one_recv, right_send, right_recv, left_send, left_recv,
    sib_send, sib_recv, q_send, q_recv, w_send, w_recv, ws_send, ws_recv,
):
    z, y, c, x = place()
    a0 = z * (1 - c) + y * c
    b0 = y * (1 - c) + z * c
    rank = z * 16 + y * 2 + c
    ring = [
        (lax.rem(z + k * c, 8), lax.rem(y + k * (1 - c), 8), c, x) for k in range(1, 8)
    ]
    right = (lax.rem(z + (1 - c), 8), lax.rem(y + c, 8), c, x)
    left = (lax.rem(z + 7 * (1 - c), 8), lax.rem(y + 7 * c, 8), c, x)
    sibling = (z, y, 1 - c, x)
    mirror = (7 - z, 7 - y, 1 - c, x)
    across = [(z, y, c, lax.rem(x + k, 4)) for k in range(1, 4)]

    own_load = pltpu.make_async_copy(own_kv, buf.at[c, a0, b0], local.at[0])
    q_load = pltpu.make_async_copy(queries.at[0], q_aug.at[0, :, pl.ds(0, 128)], local.at[1])
    own_load.start()
    q_load.start()
    greet([*ring, right, left, sibling, mirror, *across])
    own_load.wait()

    ones = [
        remote(buf.at[c, a0, b0], buf.at[c, a0, b0], one_send.at[k - 1], one_recv.at[k - 1], ring[k - 1])
        for k in range(1, 8)
    ]
    for k in (1, 7, 2, 6, 3, 5, 4):
        ones[k - 1].start()
    q_copy = remote(queries.at[1], q_aug.at[1, :, pl.ds(0, 128)], q_send, q_recv, mirror)
    q_copy.start()
    half_rows = pl.ds(pl.multiple_of(c * 128, 128), 128)
    w_copies = [
        remote(w_own.at[half_rows], w_all.at[x, half_rows], w_send.at[k], w_recv.at[k], across[k])
        for k in range(3)
    ]
    for k in (0, 2, 1):
        w_copies[k].start()

    selector = (
        (iota((4 * HALF, 128), 1) < 12)
        & (lax.rem(iota((4 * HALF, 128), 1), 4) == iota((4 * HALF, 128), 0) // HALF)
    ).astype(f32).astype(bf16)
    q_aug[0, :, 128:256] = selector
    q_aug[1, :, 128:256] = selector
    peak[...] = jnp.full(peak.shape, LOW, f32)
    accum[...] = jnp.zeros(accum.shape, f32)

    for copy in ones:
        copy.wait()

    def chunk(core, a, ch):
        return buf.at[core, a, pl.ds(ch * 4, 4)]

    def to_right(d, ch, i):
        ref = chunk(c, lax.rem(a0 - d + 8, 8), ch)
        return remote(ref, ref, right_send.at[i], right_recv.at[i], right)

    def to_left(d, ch, i):
        ref = chunk(c, lax.rem(a0 + d, 8), ch)
        return remote(ref, ref, left_send.at[i], left_recv.at[i], left)

    def to_sibling(a, ch, i):
        ref = chunk(c, a, ch)
        return remote(ref, ref, sib_send.at[i], sib_recv.at[i], sibling)

    for ch in range(2):
        to_right(0, ch, ch).start()
        to_left(0, ch, ch).start()
    for ch in range(2):
        to_sibling(a0, ch, ch).start()

    def hop(i, carry):
        d = i // 2 + 1
        ch_r = lax.rem(i, 2)
        ch_l = lax.rem(i, 2) + i // 6
        a_r = lax.rem(a0 - d + 8, 8)
        a_l = lax.rem(a0 + d, 8)
        got = chunk(c, a_r, ch_r)
        remote(got, got, right_send.at[i], right_recv.at[i], right).wait_recv()

        @pl.when(i <= 4)
        def _():
            to_right(d, ch_r, i + 2).start()

        to_sibling(a_r, ch_r, 2 + 2 * i).start()
        got = chunk(c, a_l, ch_l)
        remote(got, got, left_send.at[i], left_recv.at[i], left).wait_recv()

        @pl.when(i <= 3)
        def _():
            to_left(d, ch_l, i + 2).start()

        @pl.when(i == 5)
        def _():
            to_left(d, ch_l, 6).start()

        to_sibling(a_l, ch_l, 3 + 2 * i).start()
        return carry

    lax.fori_loop(0, 7, hop, 0)

    def drain(i, carry):
        ref = chunk(c, a0, 0)
        to_sibling(a0, 0, i).wait_recv()
        to_sibling(a0, 0, i).wait_send()
        return carry

    lax.fori_loop(0, 16, drain, 0)

    def drain_ring(i, carry):
        to_right(0, 0, i).wait_send()
        to_left(0, 0, i).wait_send()
        return carry

    lax.fori_loop(0, 7, drain_ring, 0)
    q_copy.wait()
    q_load.wait()

    def total(r, acc):
        core = lax.rem(r, 2)
        yy = lax.rem(r // 2, 8)
        zz = r // 16
        a = zz * (1 - core) + yy * core
        b = yy * (1 - core) + zz * core
        last = buf[core, a, b, HALF:ROWS, 128:256].astype(f32)[:, 127:128]
        return jnp.where(iota((16, 128), 1) == r, last, acc)

    totals = lax.fori_loop(0, 128, total, jnp.zeros((16, 128), f32))
    before = (iota((128, 128), 0) < iota((128, 128), 1)).astype(f32).astype(bf16)
    offset = jnp.dot(totals.astype(bf16), before, preferred_element_type=f32)
    offset = offset[0:8] + pltpu.roll(offset[0:8], 4, 0) + offset[8:16]
    for h in range(4):
        table[h] = jnp.broadcast_to(offset[h : h + 1], (128, 128)).T

    ones_rows = jnp.ones((16, 2 * BLOCK), bf16)
    zero_rows = jnp.zeros((112, 2 * BLOCK), bf16)

    def pair(part, core, a, j, masked):
        my_rank = rank * (1 - part) + (127 - rank) * part
        b = 2 * j

        def both(lo, hi):
            return jnp.concatenate(
                [buf[core, a, b, lo:hi, :], buf[core, a, b + 1, lo:hi, :]], axis=1
            )

        keys = both(0, HEAD)
        right_side = jnp.concatenate([keys, keys, both(HALF, ROWS), zero_rows], axis=0)
        scores = jnp.dot(q_aug[part], right_side, preferred_element_type=f32)
        sides = []
        peaks = [peak[part]]
        for u in range(2):
            their = block_rank(core, a, b + u)
            shift = jnp.concatenate(
                [
                    jnp.broadcast_to(table[h, pl.ds(their, 1), :], (HALF, 128))
                    for h in range(4)
                ],
                axis=0,
            )
            s = scores[:, u * BLOCK : (u + 1) * BLOCK]
            allowed = None
            if masked:
                q_at = my_rank * BLOCK + part * HALF + lax.rem(iota(s.shape, 0), HALF)
                k_at = their * BLOCK + iota(s.shape, 1)
                allowed = k_at <= q_at
                s = jnp.where(allowed, s, LOW)
            peaks.append(jnp.max(s, axis=1, keepdims=True) + shift)
            sides.append((s, shift, allowed))
        new_peak = jnp.maximum(jnp.maximum(peaks[0], peaks[1]), peaks[2])
        weights = []
        for s, shift, allowed in sides:
            base = new_peak - shift
            w = jnp.exp2(s - jnp.concatenate([base, base], axis=1))
            if masked:
                w = jnp.where(allowed, w, 0.0)
            weights.append(w.astype(bf16))
        values = jnp.concatenate([both(HEAD, HALF), ones_rows, zero_rows[0:48]], axis=0)
        gained = lax.dot_general(
            jnp.concatenate(weights, axis=1), values, (((1,), (1,)), ((), ())),
            preferred_element_type=f32,
        )
        accum[part] = accum[part] * jnp.exp2(peaks[0] - new_peak) + gained
        peak[part] = new_peak

    def visit(t, carry):
        part = t // 64
        u = lax.rem(t, 64)
        core = u // 32
        a = lax.rem(u // 4, 8)
        j = lax.rem(u, 4)
        my_rank = rank * (1 - part) + (127 - rank) * part
        low = block_rank(core, a, 2 * j)
        high = block_rank(core, a, 2 * j + 1)

        @pl.when(high < my_rank)
        def _():
            pair(part, core, a, j, False)

        @pl.when((low <= my_rank) & (high >= my_rank))
        def _():
            pair(part, core, a, j, True)

        return carry

    lax.fori_loop(0, 128, visit, 0)

    for part in range(2):
        total_of = accum[part]
        out = total_of[:, 0:HEAD] / total_of[:, HEAD : HEAD + 1]
        for h in range(4):
            att_out[part, :, h * HEAD : (h + 1) * HEAD] = out[h * HALF : (h + 1) * HALF].astype(bf16)

    for k in range(3):
        w_copies[k].wait()
    shared = []
    for k in range(3):
        who = lax.rem(x + 3 - k, 4)
        ref = w_all.at[who, half_rows]
        shared.append(remote(ref, ref, ws_send.at[k], ws_recv.at[k], sibling))
        shared[-1].start()
    for copy in shared:
        copy.wait()


def attend(own_kv, queries, w_output):
    vmem = pl.BlockSpec(memory_space=pltpu.VMEM)
    anyspace = pl.BlockSpec(memory_space=pl.ANY)
    dma = pltpu.SemaphoreType.DMA
    return pl.pallas_call(
        attend_kernel,
        name="attend",
        out_shape=(
            jax.ShapeDtypeStruct((2, HALF, 4 * HEAD), bf16),
            jax.ShapeDtypeStruct((4, *w_output.shape), bf16),
        ),
        in_specs=[anyspace, anyspace, anyspace],
        out_specs=(vmem, anyspace),
        scratch_shapes=[
            pltpu.VMEM((2, 8, 8, ROWS, BLOCK), bf16),
            pltpu.VMEM((2, 4 * HALF, 256), bf16),
            pltpu.VMEM((8, 128), bf16),
            pltpu.VMEM((2, 4 * HALF, 128), f32),
            pltpu.VMEM((2, 4 * HALF, 128), f32),
            pltpu.VMEM((4, 128, 128), f32),
            dma((2,)),
            dma((7,)), dma((7,)),
            dma((7,)), dma((7,)),
            dma((7,)), dma((7,)),
            dma((16,)), dma((16,)),
            dma, dma,
            dma((3,)), dma((3,)),
            dma((3,)), dma((3,)),
        ],
        compiler_params=pltpu.CompilerParams(
            collective_id=1, has_side_effects=True, vmem_limit_bytes=48 * 2**20
        ),
    )(own_kv, queries, w_output)


def output_kernel(att, w_own, w_all, out, heads, w_v, send, recv, local):
    z, y, c, x = place()
    n = 4
    here = [(z, y, c, lax.rem(x + k, n)) for k in range(1, n)]
    there = [(7 - z, 7 - y, 1 - c, g) for g in range(n)]
    loads = [pltpu.make_async_copy(w_own, w_v.at[x], local.at[0])]
    for k in range(1, n):
        g = lax.rem(x + k, n)
        loads.append(pltpu.make_async_copy(w_all.at[g], w_v.at[g], local.at[k]))
    for load in loads:
        load.start()
    greet([*here, *there])

    def to(owner):
        part = owner // 2
        device = there[owner] if part else (z, y, c, owner)
        src = att.at[part, pl.ds((owner % 2) * 64, 64), :]
        return remote(src, heads.at[x], send.at[owner], recv.at[x], device)

    for owner in range(n):
        if owner < 2:

            @pl.when(x != owner)
            def _(owner=owner):
                to(owner).start()

            @pl.when(x == owner)
            def _(owner=owner):
                heads[owner] = att[0, owner * 64 : (owner + 1) * 64, :]
        else:
            to(owner).start()

    for load in loads:
        load.wait()
    for g in range(n):
        arrives = (x >= 2) | (x != g)

        @pl.when(arrives)
        def _(g=g):
            src = att.at[0, pl.ds(0, 64), :]
            remote(src, heads.at[g], send.at[0], recv.at[g], there[0]).wait_recv()

    for col in range(0, out.shape[1], 512):
        total = None
        for g in range(n):
            part = jnp.dot(heads[g], w_v[g, :, col : col + 512], preferred_element_type=f32)
            part = part.astype(bf16).astype(f32)
            total = part if total is None else total + part
        out[:, col : col + 512] = total.astype(bf16)

    for owner in range(n):
        if owner < 2:

            @pl.when(x != owner)
            def _(owner=owner):
                to(owner).wait_send()
        else:
            to(owner).wait_send()


def output(att, w_own, w_all):
    d = w_own.shape[1]
    vmem = pl.BlockSpec(memory_space=pltpu.VMEM)
    anyspace = pl.BlockSpec(memory_space=pl.ANY)
    dma = pltpu.SemaphoreType.DMA
    return pl.pallas_call(
        output_kernel,
        name="output",
        out_shape=jax.ShapeDtypeStruct((64, d), bf16),
        in_specs=[vmem, anyspace, anyspace],
        out_specs=vmem,
        scratch_shapes=[
            pltpu.VMEM((4, 64, 4 * HEAD), bf16),
            pltpu.VMEM(w_all.shape, bf16),
            dma((4,)), dma((4,)), dma((4,)),
        ],
        compiler_params=pltpu.CompilerParams(
            collective_id=2, has_side_effects=True, vmem_limit_bytes=24 * 2**20
        ),
    )(att, w_own, w_all)


def shards(tokens, w_query, w_key, w_value, w_gate, gate_bias, w_output):
    own_kv, queries = project(
        tokens, w_query, w_key, w_value, w_gate, gate_bias.reshape(1, -1)
    )
    att, w_all = attend(own_kv, queries, w_output)
    return output(att, w_output, w_all)


def solution(mesh):
    finer = Mesh(mesh.devices.reshape(8, 8, 2, mesh.shape["tp"]), AXES)
    placed = (
        P(SP_TP, None),
        P(None, "tp"),
        P(None, "tp"),
        P(None, "tp"),
        P(None, "tp"),
        P("tp"),
        P("tp", None),
    )
    return jax.shard_map(
        shards, mesh=finer, in_specs=placed, out_specs=P(SP_TP, None), check_vma=False
    )
```

```python
import jax
import jax.numpy as jnp
from jax import lax
from jax.experimental import pallas as pl
from jax.experimental.pallas import tpu as pltpu
from jax.sharding import Mesh
from jax.sharding import PartitionSpec as P

HEAD = 64
BLOCK = 256
HALF = 128
ROWS = 144
LOG2E = 1.4426950408889634
LOW = -1e30
AXES = ("sp_0", "sp_1", "sp_2", "tp")
SP_TP = AXES
MESH = pl.DeviceIdType.MESH
f32 = jnp.float32
bf16 = jnp.bfloat16


def remote(src, dst, send, recv, device):
    return pltpu.make_async_remote_copy(
        src_ref=src, dst_ref=dst, send_sem=send, recv_sem=recv,
        device_id=device, device_id_type=MESH,
    )


def three(x):
    a = x.astype(bf16).astype(f32)
    r = x - a
    b = r.astype(bf16).astype(f32)
    return a, b, r - b


def iota(shape, dim):
    return lax.broadcasted_iota(jnp.int32, shape, dim)


def dot(a, b):
    return jnp.dot(a, b, preferred_element_type=f32)


def dot_t(a, b):
    return lax.dot_general(a, b, (((1,), (1,)), ((), ())), preferred_element_type=f32)


def block_rank(core, a, b):
    zz = a * (1 - core) + b * core
    yy = b * (1 - core) + a * core
    return zz * 16 + yy * 2 + core


def layer_kernel(
    tokens, w_q, w_kt, w_vt, w_gt, bias, w_o, out,
    x_all, wq_v, wk_v, wv_v, wg_v, bias_v, w_all, buf, sums_of, q_aug, q_far, peak, accum, table,
    att, heads,
    local, tok_send, tok_recv, one_send, one_recv, ta_send, ta_recv, tb_send, tb_recv,
    ts_send, ts_recv, right_send, right_recv, left_send, left_recv, sib_send, sib_recv,
    q_send, q_recv, w_send, w_recv, ws_send, ws_recv, att_send, att_recv,
):
    z, y, c, x = (lax.axis_index(a) for a in AXES)
    a0 = z * (1 - c) + y * c
    b0 = y * (1 - c) + z * c
    rank = z * 16 + y * 2 + c
    across = [(z, y, c, lax.rem(x + k, 4)) for k in range(1, 4)]
    ring = [(lax.rem(z + k * c, 8), lax.rem(y + k * (1 - c), 8), c, x) for k in range(1, 8)]
    cross = [(lax.rem(z + k * (1 - c), 8), lax.rem(y + k * c, 8), c, x) for k in range(1, 8)]
    right, left = cross[0], cross[6]
    sibling = (z, y, 1 - c, x)
    mirrors = [(7 - z, 7 - y, 1 - c, g) for g in range(4)]
    mirror = (7 - z, 7 - y, 1 - c, x)

    loads = [
        pltpu.make_async_copy(src, dst, local.at[i])
        for i, (src, dst) in enumerate((
            (tokens, x_all.at[x]), (w_kt, wk_v), (w_vt, wv_v), (w_gt, wg_v), (bias, bias_v),
            (w_q, wq_v), (w_o, w_all.at[x]),
        ))
    ]
    for load in loads:
        load.start()
    barrier = pltpu.get_barrier_semaphore()
    peers = [*mirrors, *cross, *ring, *across, sibling]
    for peer in peers:
        pl.semaphore_signal(barrier, inc=1, device_id=peer, device_id_type=MESH)
    loads[0].wait()
    pl.semaphore_wait(barrier, len(peers))

    toks = [remote(x_all.at[x], x_all.at[x], tok_send.at[k], tok_recv.at[k], across[k]) for k in range(3)]
    for k in (0, 2, 1):
        toks[k].start()

    lanes = iota((4 * HALF, 128), 1)
    selector = (
        (lanes < 12) & (lax.rem(lanes, 4) == iota((4 * HALF, 128), 0) // HALF)
    ).astype(f32).astype(bf16)
    q_aug[0, :, 128:256] = selector
    q_aug[1, :, 128:256] = selector
    peak[...] = jnp.full(peak.shape, LOW, f32)
    accum[...] = jnp.zeros(accum.shape, f32)
    for load in loads[1:]:
        load.wait()
    for k in range(3):
        toks[k].wait_recv()

    rows = x_all[...].reshape(BLOCK, x_all.shape[2])
    gates = dot_t(wg_v[...], rows).astype(bf16).astype(f32)
    spread = jnp.broadcast_to(bias_v[...], (4, 4))
    column = jnp.sum(jnp.where(iota((4, 4), 0) == iota((4, 4), 1), spread, 0.0), axis=1, keepdims=True)
    gates = jnp.concatenate([gates + column, jnp.zeros((4, BLOCK), f32)], axis=0)
    buf[c, a0, b0, 0:HEAD, :] = dot_t(wk_v[...], rows).astype(bf16)
    buf[c, a0, b0, HEAD:HALF, :] = dot_t(wv_v[...], rows).astype(bf16)
    small = jnp.exp(-jnp.abs(gates))
    series = small * (1.0 - small * (0.5 - small * (1 / 3 - small * (0.25 - small * 0.2))))
    logs = jnp.minimum(gates, 0.0) - jnp.where(small < 0.02, series, jnp.log(1.0 + small))
    tri = (iota((BLOCK, BLOCK), 0) <= iota((BLOCK, BLOCK), 1)).astype(f32).astype(bf16)
    pieces = jnp.concatenate([*three(logs), jnp.zeros((8, BLOCK), f32)], axis=0)
    sums = dot(pieces.astype(bf16), tri)
    decay = (sums[0:8] + sums[8:16] + sums[16:24]) * (-LOG2E)
    hi, mid, lo = three(decay)
    row = iota((8, BLOCK), 0)
    first = jnp.where(row < 4, hi, pltpu.roll(mid, 4, 0))
    second = jnp.where(row < 4, lo, 0.0)
    last = jnp.broadcast_to(decay[:, BLOCK - 1 : BLOCK], (8, 128))
    ends = jnp.where((iota((8, 128), 0) == iota((8, 128), 1)) & (iota((8, 128), 0) < 4), last, 0.0)
    sums_of[c, a0, b0] = jnp.sum(ends, axis=0, keepdims=True)
    buf[c, a0, b0, HALF:ROWS, :] = jnp.concatenate([first, second], axis=0).astype(bf16)

    own_sum = sums_of.at[c, a0, b0]
    tas = [remote(own_sum, own_sum, ta_send.at[k], ta_recv.at[k], ring[k]) for k in range(7)]
    for k in range(7):
        tas[k].start()
    own = buf.at[c, a0, b0]
    ones = [remote(own, own, one_send.at[k], one_recv.at[k], ring[k]) for k in range(7)]
    for k in (0, 6, 1, 5, 2, 4, 3):
        ones[k].start()

    queries = dot(rows, wq_v[...]).astype(bf16).astype(f32) * (LOG2E * HEAD**-0.5)
    top = queries.astype(bf16).astype(f32)
    rest = queries - top
    for h in range(4):
        cols = slice(h * HEAD, (h + 1) * HEAD)
        both = jnp.concatenate([top[:, cols], rest[:, cols]], axis=1).astype(bf16)
        q_aug[0, h * HALF : (h + 1) * HALF, 0:128] = both[0:HALF]
        q_far[h * HALF : (h + 1) * HALF, :] = both[HALF:]
    for k in range(3):
        toks[k].wait_send()
    q_copy = remote(q_far, q_aug.at[1, :, pl.ds(0, 128)], q_send, q_recv, mirror)
    q_copy.start()
    half_rows = pl.ds(pl.multiple_of(c * 128, 128), 128)
    own_half = w_all.at[x, half_rows]
    w_copies = [remote(own_half, own_half, w_send.at[k], w_recv.at[k], across[k]) for k in range(3)]
    for k in (0, 2, 1):
        w_copies[k].start()

    for k in range(7):
        tas[k].wait()
    eight = sums_of.at[c, a0]
    tbs = [remote(eight, eight, tb_send.at[k], tb_recv.at[k], cross[k]) for k in range(7)]
    for k in range(7):
        tbs[k].start()

    def chunk(core, a, ch):
        return buf.at[core, a, pl.ds(ch * 4, 4)]

    def to_right(d, ch, i):
        ref = chunk(c, lax.rem(a0 - d + 8, 8), ch)
        return remote(ref, ref, right_send.at[i], right_recv.at[i], right)

    def to_left(d, ch, i):
        ref = chunk(c, lax.rem(a0 + d, 8), ch)
        return remote(ref, ref, left_send.at[i], left_recv.at[i], left)

    def to_sibling(a, ch, i):
        ref = chunk(c, a, ch)
        return remote(ref, ref, sib_send.at[i], sib_recv.at[i], sibling)

    for k in range(7):
        ones[k].wait()
    for ch in range(2):
        to_right(0, ch, ch).start()
        to_left(0, ch, ch).start()
    for ch in range(2):
        to_sibling(a0, ch, ch).start()

    for k in range(7):
        tbs[k].wait()
    core_sums = sums_of.at[c]
    share = remote(core_sums, core_sums, ts_send, ts_recv, sibling)
    share.start()
    q_copy.wait()
    share.wait()

    def slot_rank(dim):
        s = iota((128, 128), dim)
        core = s // 64
        a = lax.rem(s // 8, 8)
        b = lax.rem(s, 8)
        return block_rank(core, a, b)

    before = (slot_rank(1) < slot_rank(0)).astype(f32).astype(bf16)
    all_sums = sums_of[...].reshape(128, 128)
    offset = None
    for piece in three(all_sums):
        part_of = dot(before, piece.astype(bf16))
        offset = part_of if offset is None else offset + part_of
    for h in range(4):
        table[h] = jnp.broadcast_to(offset[:, h : h + 1], (128, 128))

    def tile(part, core, a, b, count, masked):
        keys = count * BLOCK

        def joined(lo, hi):
            return jnp.concatenate([buf[core, a, b + u, lo:hi, :] for u in range(count)], axis=1)

        k_t = joined(0, HEAD)
        right_side = jnp.concatenate(
            [k_t, k_t, joined(HALF, ROWS), jnp.zeros((112, keys), bf16)], axis=0
        )
        scores = dot(q_aug[part], right_side)
        allowed = None
        if masked:
            q_at = part * HALF + lax.rem(iota((4 * HALF, BLOCK), 0), HALF)
            allowed = iota((4 * HALF, BLOCK), 1) <= q_at
            scores = jnp.where(allowed, scores, LOW)
        shifts = []
        highest = None
        for u in range(count):
            slot = core * 64 + a * 8 + b + u
            shift = jnp.concatenate(
                [jnp.broadcast_to(table[h, pl.ds(slot, 1), :], (HALF, 128)) for h in range(4)],
                axis=0,
            )
            s = scores[:, u * BLOCK : (u + 1) * BLOCK]
            most = jnp.maximum(s[:, 0:128], s[:, 128:256]) + shift
            highest = most if highest is None else jnp.maximum(highest, most)
            shifts.append(shift)
        old = peak[part]
        new = jnp.maximum(old, jnp.max(highest, axis=1, keepdims=True))
        weights = []
        for u in range(count):
            base = new - shifts[u]
            for v in range(2):
                at = u * BLOCK + v * 128
                w = jnp.exp2(scores[:, at : at + 128] - base)
                if masked:
                    w = jnp.where(allowed[:, v * 128 : (v + 1) * 128], w, 0.0)
                weights.append(w.astype(bf16))
        v_t = jnp.concatenate(
            [joined(HEAD, HALF), jnp.ones((16, keys), bf16), jnp.zeros((48, keys), bf16)], axis=0
        )
        gained = dot_t(jnp.concatenate(weights, axis=1), v_t)
        accum[part] = accum[part] * jnp.exp2(old - new) + gained
        peak[part] = new

    def process(core, a, ch):
        def one_part(part, carry):
            mine = rank * (1 - part) + (127 - rank) * part
            b = ch * 4
            ranks = [block_rank(core, a, b + u) for u in range(4)]
            full = sum((r < mine).astype(jnp.int32) for r in ranks)
            equal = sum((r == mine).astype(jnp.int32) for r in ranks)

            @pl.when(full == 4)
            def _():
                tile(part, core, a, b, 4, False)

            @pl.when((full == 2) | (full == 3))
            def _():
                tile(part, core, a, b, 2, False)

            @pl.when((full == 1) | (full == 3))
            def _():
                tile(part, core, a, b + full - 1, 1, False)

            @pl.when(equal == 1)
            def _():
                tile(part, core, a, b + full, 1, True)

            return carry

        lax.fori_loop(0, 2, one_part, 0)

    def w_share(k):
        ref = w_all.at[lax.rem(x + 3 - k, 4), half_rows]
        return remote(ref, ref, ws_send.at[k], ws_recv.at[k], sibling)

    def step(t, carry):
        i = t // 4 - 1
        sel = lax.rem(t, 4)
        d = (i + 2) // 2
        side = lax.rem(sel, 2)
        ch = (lax.rem(i + 2, 2) + (i // 6) * side) * jnp.minimum(i + 1, 1) + side * (
            1 - jnp.minimum(i + 1, 1)
        )

        @pl.when((sel == 0) & (i >= 0))
        def _():
            to_right(0, 0, i).wait_recv()

            @pl.when(i <= 4)
            def _():
                to_right(d, ch, i + 2).start()

            to_sibling(lax.rem(a0 - d + 8, 8), ch, 2 + 2 * i).start()

        @pl.when((sel == 1) & (i >= 0))
        def _():
            to_left(0, 0, i).wait_recv()

            @pl.when(i <= 3)
            def _():
                to_left(d, ch, i + 2).start()

            @pl.when(i == 5)
            def _():
                to_left(d, ch, 6).start()

            to_sibling(lax.rem(a0 + d, 8), ch, 3 + 2 * i).start()

        @pl.when(sel >= 2)
        def _():
            to_sibling(a0, 0, 2 * i + sel).wait_recv()

        @pl.when(t == 20)
        def _():
            for k in range(3):
                w_copies[k].wait()
                w_share(k).start()

        core = c * (1 - sel // 2) + (1 - c) * (sel // 2)
        center = a0 * (1 - sel // 2) + b0 * (sel // 2)
        a = lax.rem(center + 8 + d * (2 * side - 1), 8)
        process(core, a, ch)
        return carry

    lax.fori_loop(0, 32, step, 0)

    for part in range(2):
        total_of = accum[part]
        result = total_of[:, 0:HEAD] / total_of[:, HEAD : HEAD + 1]
        for h in range(4):
            att[part, :, h * HEAD : (h + 1) * HEAD] = result[h * HALF : (h + 1) * HALF].astype(bf16)

    def drain(i, carry):
        to_sibling(a0, 0, i).wait_send()
        return carry

    lax.fori_loop(0, 16, drain, 0)

    def drain_ring(i, carry):
        to_right(0, 0, i).wait_send()
        to_left(0, 0, i).wait_send()
        return carry

    lax.fori_loop(0, 7, drain_ring, 0)

    def to(owner):
        part = owner // 2
        device = mirrors[owner] if part else (z, y, c, owner)
        src = att.at[part, pl.ds((owner % 2) * 64, 64), :]
        return remote(src, heads.at[x], att_send.at[owner], att_recv.at[x], device)

    for owner in (2, 3):
        to(owner).start()
    for owner in range(2):

        @pl.when(x != owner)
        def _(owner=owner):
            to(owner).start()

        @pl.when(x == owner)
        def _(owner=owner):
            heads[owner] = att[0, owner * 64 : (owner + 1) * 64, :]

    for k in range(3):
        w_share(k).wait()
    for g in range(4):

        @pl.when((x >= 2) | (x != g))
        def _(g=g):
            src = att.at[0, pl.ds(0, 64), :]
            remote(src, heads.at[g], att_send.at[0], att_recv.at[g], mirrors[0]).wait_recv()

    for col in range(0, out.shape[1], 512):
        total = None
        for g in range(4):
            part = dot(heads[g], w_all[g, :, col : col + 512]).astype(bf16).astype(f32)
            total = part if total is None else total + part
        out[:, col : col + 512] = total.astype(bf16)

    for owner in range(4):
        if owner < 2:

            @pl.when(x != owner)
            def _(owner=owner):
                to(owner).wait_send()
        else:
            to(owner).wait_send()


def shards(tokens, w_query, w_key, w_value, w_gate, gate_bias, w_output):
    d = tokens.shape[1]
    hbm = pl.BlockSpec(memory_space=pltpu.HBM)
    dma = pltpu.SemaphoreType.DMA
    vmem = pltpu.VMEM
    return pl.pallas_call(
        layer_kernel,
        name="layer",
        out_shape=jax.ShapeDtypeStruct(tokens.shape, bf16),
        in_specs=[hbm] * 7,
        out_specs=pl.BlockSpec(memory_space=pltpu.VMEM),
        scratch_shapes=[
            vmem((4, *tokens.shape), bf16),
            vmem(w_query.shape, bf16),
            vmem((HEAD, d), bf16),
            vmem((HEAD, d), bf16),
            vmem((4, d), bf16),
            vmem((1, 4), f32),
            vmem((4, *w_output.shape), bf16),
            vmem((2, 8, 8, ROWS, BLOCK), bf16),
            vmem((2, 8, 8, 1, 128), f32),
            vmem((2, 4 * HALF, 256), bf16),
            vmem((4 * HALF, 128), bf16),
            vmem((2, 4 * HALF, 128), f32),
            vmem((2, 4 * HALF, 128), f32),
            vmem((4, 128, 128), f32),
            vmem((2, HALF, 4 * HEAD), bf16),
            vmem((4, 64, 4 * HEAD), bf16),
            dma((7,)),
            dma((3,)), dma((3,)),
            dma((7,)), dma((7,)),
            dma((7,)), dma((7,)),
            dma((7,)), dma((7,)),
            dma, dma,
            dma((7,)), dma((7,)),
            dma((7,)), dma((7,)),
            dma((16,)), dma((16,)),
            dma, dma,
            dma((3,)), dma((3,)),
            dma((3,)), dma((3,)),
            dma((4,)), dma((4,)),
        ],
        compiler_params=pltpu.CompilerParams(
            collective_id=0, has_side_effects=True, vmem_limit_bytes=56 * 2**20
        ),
    )(tokens, w_query, w_key.T, w_value.T, w_gate.T, gate_bias.reshape(1, -1), w_output)


def solution(mesh):
    finer = Mesh(mesh.devices.reshape(8, 8, 2, mesh.shape["tp"]), AXES)
    placed = (
        P(SP_TP, None),
        P(None, "tp"),
        P(None, "tp"),
        P(None, "tp"),
        P(None, "tp"),
        P("tp"),
        P("tp", None),
    )
    return jax.shard_map(
        shards, mesh=finer, in_specs=placed, out_specs=P(SP_TP, None), check_vma=False
    )
```

```python
import jax
import jax.numpy as jnp
from jax import lax
from jax.experimental import pallas as pl
from jax.experimental.pallas import tpu as pltpu
from jax.sharding import Mesh
from jax.sharding import PartitionSpec as P

HEAD = 64
BLOCK = 256
HALF = 128
ROWS = 144
LOG2E = 1.4426950408889634
LOW = -1e30
AXES = ("sp_0", "sp_1", "sp_2", "tp")
SP_TP = AXES
MESH = pl.DeviceIdType.MESH
f32 = jnp.float32
bf16 = jnp.bfloat16


def remote(src, dst, send, recv, device):
    return pltpu.make_async_remote_copy(
        src_ref=src, dst_ref=dst, send_sem=send, recv_sem=recv,
        device_id=device, device_id_type=MESH,
    )


def three(x):
    a = x.astype(bf16).astype(f32)
    r = x - a
    b = r.astype(bf16).astype(f32)
    return a, b, r - b


def iota(shape, dim):
    return lax.broadcasted_iota(jnp.int32, shape, dim)


def dot(a, b):
    return jnp.dot(a, b, preferred_element_type=f32)


def dot_t(a, b):
    return lax.dot_general(a, b, (((1,), (1,)), ((), ())), preferred_element_type=f32)


def block_rank(core, a, b):
    zz = a * (1 - core) + b * core
    yy = b * (1 - core) + a * core
    return zz * 16 + yy * 2 + core


def layer_kernel(
    tokens, w_q, w_kt, w_vt, w_gt, bias, w_o, out,
    x_all, wq_v, wk_v, wv_v, wg_v, bias_v, w_all, buf, sums_of, q_aug, q_far, q_near, peak, accum, table,
    att, heads,
    local, tok_send, tok_recv, one_send, one_recv, ta_send, ta_recv, tb_send, tb_recv,
    ts_send, ts_recv, right_send, right_recv, left_send, left_recv, sib_send, sib_recv,
    q_send, q_recv, w_send, w_recv, ws_send, ws_recv, att_send, att_recv,
):
    z, y, c, x = (lax.axis_index(a) for a in AXES)
    a0 = z * (1 - c) + y * c
    b0 = y * (1 - c) + z * c
    my_slot = c * 64 + a0 * 8 + b0
    rank = z * 16 + y * 2 + c
    across = [(z, y, c, lax.rem(x + k, 4)) for k in range(1, 4)]
    ring = [(lax.rem(z + k * c, 8), lax.rem(y + k * (1 - c), 8), c, x) for k in range(1, 8)]
    cross = [(lax.rem(z + k * (1 - c), 8), lax.rem(y + k * c, 8), c, x) for k in range(1, 8)]
    right, left = cross[0], cross[6]
    sibling = (z, y, 1 - c, x)
    mirrors = [(7 - z, y, 1 - c, g) for g in range(4)]
    mirror = (7 - z, y, 1 - c, x)
    far_rank = (7 - z) * 16 + y * 2 + 1 - c

    loads = [
        pltpu.make_async_copy(src, dst, local.at[i])
        for i, (src, dst) in enumerate((
            (tokens, x_all.at[x]), (w_kt, wk_v), (w_vt, wv_v), (w_gt, wg_v), (bias, bias_v),
            (w_q, wq_v), (w_o, w_all.at[x]),
        ))
    ]
    for load in loads:
        load.start()
    barrier = pltpu.get_barrier_semaphore()
    peers = [*mirrors, *cross, *ring, *across, sibling]
    for peer in peers:
        pl.semaphore_signal(barrier, inc=1, device_id=peer, device_id_type=MESH)
    loads[0].wait()
    pl.semaphore_wait(barrier, len(peers))

    def piece(owner, half):
        return x_all.at[owner, pl.ds(half * 32, 32)]

    def tok(i):
        half = (0, 1, 1, 0, 0, 1)[i]
        owner = (x, x, x, x, lax.rem(x + 3, 4), lax.rem(x + 1, 4))[i]
        ref = piece(owner, half)
        return remote(ref, ref, tok_send.at[i], tok_recv.at[i], across[(0, 0, 2, 2, 0, 2)[i]])

    for i in (0, 2, 1, 3):
        tok(i).start()

    for i in (0, 2):
        tok(i).wait_recv()
        tok(4 + i // 2).start()
    buf[128] = jnp.zeros((ROWS, BLOCK), bf16)
    lanes = iota((4 * HALF, 128), 1)
    selector = (
        (lanes < 12) & (lax.rem(lanes, 4) == iota((4 * HALF, 128), 0) // HALF)
    ).astype(f32).astype(bf16)
    q_aug[0, :, 128:256] = selector
    q_aug[1, :, 128:256] = selector
    peak[...] = jnp.full(peak.shape, LOW, f32)
    accum[...] = jnp.zeros(accum.shape, f32)
    for load in loads[1:]:
        load.wait()
    for i in (1, 3, 4, 5):
        tok(i).wait_recv()

    rows = x_all[...].reshape(BLOCK, x_all.shape[2])
    gates = dot_t(wg_v[...], rows).astype(bf16).astype(f32)
    spread = jnp.broadcast_to(bias_v[...], (4, 4))
    column = jnp.sum(jnp.where(iota((4, 4), 0) == iota((4, 4), 1), spread, 0.0), axis=1, keepdims=True)
    gates = jnp.concatenate([gates + column, jnp.zeros((4, BLOCK), f32)], axis=0)
    buf[my_slot, 0:HEAD, :] = dot_t(wk_v[...], rows).astype(bf16)
    buf[my_slot, HEAD:HALF, :] = dot_t(wv_v[...], rows).astype(bf16)
    small = jnp.exp(-jnp.abs(gates))
    series = small * (1.0 - small * (0.5 - small * (1 / 3 - small * (0.25 - small * 0.2))))
    logs = jnp.minimum(gates, 0.0) - jnp.where(small < 0.02, series, jnp.log(1.0 + small))
    tri = (iota((BLOCK, BLOCK), 0) <= iota((BLOCK, BLOCK), 1)).astype(f32).astype(bf16)
    pieces = jnp.concatenate([*three(logs), jnp.zeros((8, BLOCK), f32)], axis=0)
    sums = dot(pieces.astype(bf16), tri)
    decay = (sums[0:8] + sums[8:16] + sums[16:24]) * (-LOG2E)
    hi, mid, lo = three(decay)
    row = iota((8, BLOCK), 0)
    first = jnp.where(row < 4, hi, pltpu.roll(mid, 4, 0))
    second = jnp.where(row < 4, lo, 0.0)
    last = jnp.broadcast_to(decay[:, BLOCK - 1 : BLOCK], (8, 128))
    ends = jnp.where((iota((8, 128), 0) == iota((8, 128), 1)) & (iota((8, 128), 0) < 4), last, 0.0)
    sums_of[c, a0, b0] = jnp.sum(ends, axis=0, keepdims=True)
    buf[my_slot, HALF:ROWS, :] = jnp.concatenate([first, second], axis=0).astype(bf16)

    own_sum = sums_of.at[c, a0, b0]
    tas = [remote(own_sum, own_sum, ta_send.at[k], ta_recv.at[k], ring[k]) for k in range(7)]
    for k in range(7):
        tas[k].start()
    own = buf.at[my_slot]
    ones = [remote(own, own, one_send.at[k], one_recv.at[k], ring[k]) for k in range(7)]
    for k in (3, 2, 4, 1, 5, 0, 6):
        ones[k].start()

    queries = dot(rows, wq_v[...]).astype(bf16)
    q_far[...] = queries[HALF:]

    def expand(part, raw):
        scaled = raw.astype(f32) * (LOG2E * HEAD**-0.5)
        top = scaled.astype(bf16).astype(f32)
        rest = scaled - top
        for h in range(4):
            cols = slice(h * HEAD, (h + 1) * HEAD)
            both = jnp.concatenate([top[:, cols], rest[:, cols]], axis=1)
            q_aug[part, h * HALF : (h + 1) * HALF, 0:128] = both.astype(bf16)

    expand(0, queries[0:HALF])
    for i in range(6):
        tok(i).wait_send()
    q_copy = remote(q_far, q_near, q_send, q_recv, mirror)
    q_copy.start()
    half_rows = pl.ds(pl.multiple_of(c * 128, 128), 128)
    own_half = w_all.at[x, half_rows]
    w_copies = [remote(own_half, own_half, w_send.at[k], w_recv.at[k], across[k]) for k in range(3)]
    for k in (0, 2, 1):
        w_copies[k].start()

    for k in range(7):
        tas[k].wait()
    eight = sums_of.at[c, a0]
    tbs = [remote(eight, eight, tb_send.at[k], tb_recv.at[k], cross[k]) for k in range(7)]
    for k in range(7):
        tbs[k].start()

    def chunk(core, a, ch):
        return buf.at[pl.ds(core * 64 + a * 8 + ch * 4, 4)]

    def to_right(d, ch, i):
        ref = chunk(c, lax.rem(a0 - d + 8, 8), ch)
        return remote(ref, ref, right_send.at[i], right_recv.at[i], right)

    def to_left(d, ch, i):
        ref = chunk(c, lax.rem(a0 + d, 8), ch)
        return remote(ref, ref, left_send.at[i], left_recv.at[i], left)

    def to_sibling(a, ch, i):
        ref = chunk(c, a, ch)
        return remote(ref, ref, sib_send.at[i], sib_recv.at[i], sibling)

    for k in range(7):
        ones[k].wait()
    for ch in range(2):
        to_right(0, ch, ch).start()
        to_left(0, 1 - ch, ch).start()
    for ch in range(2):
        to_sibling(a0, ch, ch).start()

    for k in range(7):
        tbs[k].wait()
    core_sums = sums_of.at[c]
    share = remote(core_sums, core_sums, ts_send, ts_recv, sibling)
    share.start()
    q_copy.wait()
    expand(1, q_near[...])
    share.wait()

    def slot_rank(dim):
        s = iota((128, 128), dim)
        core = s // 64
        a = lax.rem(s // 8, 8)
        b = lax.rem(s, 8)
        return block_rank(core, a, b)

    before = (slot_rank(1) < slot_rank(0)).astype(f32).astype(bf16)
    all_sums = sums_of[...].reshape(128, 128)
    offset = None
    for piece in three(all_sums):
        part_of = dot(before, piece.astype(bf16))
        offset = part_of if offset is None else offset + part_of
    for h in range(4):
        table[h, 0:128] = jnp.broadcast_to(offset[:, h : h + 1], (128, 128))
        table[h, 128:136] = jnp.full((8, 128), LOW, f32)

    def tile(part, slots, masked):
        count = len(slots)
        keys = count * BLOCK

        def joined(lo, hi):
            return jnp.concatenate([buf[slot, lo:hi, :] for slot in slots], axis=1)

        k_t = joined(0, HEAD)
        right_side = jnp.concatenate(
            [k_t, k_t, joined(HALF, ROWS), jnp.zeros((112, keys), bf16)], axis=0
        )
        scores = dot(q_aug[part], right_side)
        allowed = None
        if masked:
            q_at = part * HALF + lax.rem(iota((4 * HALF, BLOCK), 0), HALF)
            allowed = iota((4 * HALF, BLOCK), 1) <= q_at
            scores = jnp.where(allowed, scores, LOW)
        shifts = []
        highest = None
        for u in range(count):
            shift = jnp.concatenate(
                [jnp.broadcast_to(table[h, pl.ds(slots[u], 1), :], (HALF, 128)) for h in range(4)],
                axis=0,
            )
            s = scores[:, u * BLOCK : (u + 1) * BLOCK]
            most = jnp.maximum(s[:, 0:128], s[:, 128:256]) + shift
            highest = most if highest is None else jnp.maximum(highest, most)
            shifts.append(shift)
        old = peak[part]
        new = jnp.maximum(old, jnp.max(highest, axis=1, keepdims=True))
        weights = []
        for u in range(count):
            base = new - shifts[u]
            for v in range(2):
                at = u * BLOCK + v * 128
                w = jnp.exp2(scores[:, at : at + 128] - base)
                if masked:
                    w = jnp.where(allowed[:, v * 128 : (v + 1) * 128], w, 0.0)
                weights.append(w.astype(bf16))
        v_t = jnp.concatenate(
            [joined(HEAD, HALF), jnp.ones((16, keys), bf16), jnp.zeros((48, keys), bf16)], axis=0
        )
        gained = dot_t(jnp.concatenate(weights, axis=1), v_t)
        accum[part] = accum[part] * jnp.exp2(old - new) + gained
        peak[part] = new

    def w_share(k):
        ref = w_all.at[lax.rem(x + 3 - k, 4), half_rows]
        return remote(ref, ref, ws_send.at[k], ws_recv.at[k], sibling)

    def arrival(i, side, core):
        d = (i + 2) // 2
        later = jnp.minimum(i + 1, 1)
        odd = lax.rem(i + 2, 2)
        ch = (odd * (1 - side) + (1 - odd) * side) * later + side * (1 - later)
        center = z * (1 - core) + y * core
        return lax.rem(center + 8 + d * (2 * side - 1), 8), ch

    owners = (rank, far_rank)
    diagonals = (
        my_slot,
        (1 - c) * 64 + ((7 - z) * c + y * (1 - c)) * 8 + y * c + (7 - z) * (1 - c),
    )

    def needed(n):
        starts = []
        numbers = ([], [])
        for i, core, live in ((n - 1, c, n <= 7), (n - 2, 1 - c, n >= 1)):
            at = jnp.maximum(jnp.minimum(i, 6), -1)
            for side in range(2):
                a, ch = arrival(at, side, core)
                starts.append(core * 64 + a * 8 + ch * 4)
                for part in range(2):
                    whole = sum(
                        (block_rank(core, a, ch * 4 + u) < owners[part]).astype(jnp.int32)
                        for u in range(4)
                    )
                    numbers[part].append(whole * live.astype(jnp.int32))
        return starts, numbers

    def pick(k, starts, number):
        first, second = number[0], number[0] + number[1]
        third = second + number[2]
        fourth = third + number[3]
        slot = jnp.where(k < third, starts[2] + k - second, starts[3] + k - third)
        slot = jnp.where(k < second, starts[1] + k - first, slot)
        slot = jnp.where(k < first, starts[0] + k, slot)
        return jnp.where(k < fourth, slot, 128)

    def round_of(n, kept):
        i = n - 1

        @pl.when((n >= 1) & (n <= 7))
        def _():
            d = (i + 2) // 2
            a_r, ch_r = arrival(i, 0, c)
            a_l, ch_l = arrival(i, 1, c)
            to_right(0, 0, i).wait_recv()

            @pl.when(i <= 4)
            def _():
                to_right(d, ch_r, i + 2).start()

            to_left(0, 0, i).wait_recv()

            @pl.when(i <= 4)
            def _():
                to_left(d, ch_l, i + 2).start()

            to_sibling(a_r, ch_r, 2 + 2 * i).start()
            to_sibling(a_l, ch_l, 3 + 2 * i).start()

        @pl.when(n >= 1)
        def _():
            to_sibling(a0, 0, 2 * i).wait_recv()
            to_sibling(a0, 0, 2 * i + 1).wait_recv()

        @pl.when(n == 6)
        def _():
            for k in range(3):
                w_copies[k].wait()
                w_share(k).start()

        @pl.when((n == 0) | (n == 7))
        def _():
            part = n // 7
            tile(part, [diagonals[0] * (1 - part) + diagonals[1] * part], True)

        starts, numbers = needed(n)
        fresh = [sum(numbers[part]) for part in range(2)]
        tiles = [(kept[part][0] + fresh[part] + 7 * (n // 8)) // 8 for part in range(2)]

        def one_tile(k, carry):
            part = (k >= tiles[0]).astype(jnp.int32)
            first = (k - part * tiles[0]) * 8
            number = [numbers[0][q] * (1 - part) + numbers[1][q] * part for q in range(4)]
            held = [kept[0][q] * (1 - part) + kept[1][q] * part for q in range(8)]
            slots = []
            for u in range(8):
                slot = pick(first + u - held[0], starts, number)
                if u < 7:
                    slot = jnp.where(first + u < held[0], held[1 + u], slot)
                slots.append(slot)
            tile(part, slots, False)
            return carry

        lax.fori_loop(0, tiles[0] + tiles[1], one_tile, 0)
        after = []
        for part in range(2):
            first = tiles[part] * 8
            rest = [jnp.maximum(kept[part][0] + fresh[part] - first, 0)]
            for u in range(7):
                slot = pick(first + u - kept[part][0], starts, numbers[part])
                rest.append(jnp.where(first + u < kept[part][0], kept[part][1 + u], slot))
            after.append(tuple(rest))
        return tuple(after)

    nothing = tuple(jnp.int32(0) for _ in range(8))
    lax.fori_loop(0, 9, round_of, (nothing, nothing))

    for part in range(2):
        total_of = accum[part]
        result = total_of[:, 0:HEAD] / total_of[:, HEAD : HEAD + 1]
        for h in range(4):
            att[part, :, h * HEAD : (h + 1) * HEAD] = result[h * HALF : (h + 1) * HALF].astype(bf16)

    def drain(i, carry):
        to_sibling(a0, 0, i).wait_send()
        return carry

    lax.fori_loop(0, 16, drain, 0)

    def drain_ring(i, carry):
        to_right(0, 0, i).wait_send()
        to_left(0, 0, i).wait_send()
        return carry

    lax.fori_loop(0, 7, drain_ring, 0)

    def to(owner):
        part = owner // 2
        device = mirrors[owner] if part else (z, y, c, owner)
        src = att.at[part, pl.ds((owner % 2) * 64, 64), :]
        return remote(src, heads.at[x], att_send.at[owner], att_recv.at[x], device)

    for owner in (2, 3):
        to(owner).start()
    for owner in range(2):

        @pl.when(x != owner)
        def _(owner=owner):
            to(owner).start()

        @pl.when(x == owner)
        def _(owner=owner):
            heads[owner] = att[0, owner * 64 : (owner + 1) * 64, :]

    for k in range(3):
        w_share(k).wait()
    for g in range(4):

        @pl.when((x >= 2) | (x != g))
        def _(g=g):
            src = att.at[0, pl.ds(0, 64), :]
            remote(src, heads.at[g], att_send.at[0], att_recv.at[g], mirrors[0]).wait_recv()

    for col in range(0, out.shape[1], 512):
        total = None
        for g in range(4):
            part = dot(heads[g], w_all[g, :, col : col + 512]).astype(bf16).astype(f32)
            total = part if total is None else total + part
        out[:, col : col + 512] = total.astype(bf16)

    for owner in range(4):
        if owner < 2:

            @pl.when(x != owner)
            def _(owner=owner):
                to(owner).wait_send()
        else:
            to(owner).wait_send()


def shards(tokens, w_query, w_key, w_value, w_gate, gate_bias, w_output):
    d = tokens.shape[1]
    hbm = pl.BlockSpec(memory_space=pltpu.HBM)
    dma = pltpu.SemaphoreType.DMA
    vmem = pltpu.VMEM
    return pl.pallas_call(
        layer_kernel,
        name="layer",
        out_shape=jax.ShapeDtypeStruct(tokens.shape, bf16),
        in_specs=[hbm] * 7,
        out_specs=pl.BlockSpec(memory_space=pltpu.VMEM),
        scratch_shapes=[
            vmem((4, *tokens.shape), bf16),
            vmem(w_query.shape, bf16),
            vmem((HEAD, d), bf16),
            vmem((HEAD, d), bf16),
            vmem((4, d), bf16),
            vmem((1, 4), f32),
            vmem((4, *w_output.shape), bf16),
            vmem((129, ROWS, BLOCK), bf16),
            vmem((2, 8, 8, 1, 128), f32),
            vmem((2, 4 * HALF, 256), bf16),
            vmem((HALF, 4 * HEAD), bf16),
            vmem((HALF, 4 * HEAD), bf16),
            vmem((2, 4 * HALF, 128), f32),
            vmem((2, 4 * HALF, 128), f32),
            vmem((4, 136, 128), f32),
            vmem((2, HALF, 4 * HEAD), bf16),
            vmem((4, 64, 4 * HEAD), bf16),
            dma((7,)),
            dma((6,)), dma((6,)),
            dma((7,)), dma((7,)),
            dma((7,)), dma((7,)),
            dma((7,)), dma((7,)),
            dma, dma,
            dma((7,)), dma((7,)),
            dma((7,)), dma((7,)),
            dma((16,)), dma((16,)),
            dma, dma,
            dma((3,)), dma((3,)),
            dma((3,)), dma((3,)),
            dma((4,)), dma((4,)),
        ],
        compiler_params=pltpu.CompilerParams(
            collective_id=0, has_side_effects=True, vmem_limit_bytes=56 * 2**20
        ),
    )(tokens, w_query, w_key.T, w_value.T, w_gate.T, gate_bias.reshape(1, -1), w_output)


def solution(mesh):
    finer = Mesh(mesh.devices.reshape(8, 8, 2, mesh.shape["tp"]), AXES)
    placed = (
        P(SP_TP, None),
        P(None, "tp"),
        P(None, "tp"),
        P(None, "tp"),
        P(None, "tp"),
        P("tp"),
        P("tp", None),
    )
    return jax.shard_map(
        shards, mesh=finer, in_specs=placed, out_specs=P(SP_TP, None), check_vma=False
    )
```

```python
import jax
import jax.numpy as jnp
from jax import lax
from jax.experimental import pallas as pl
from jax.experimental.pallas import tpu as pltpu
from jax.sharding import Mesh
from jax.sharding import PartitionSpec as P

HEAD = 64
BLOCK = 256
HALF = 128
ROWS = 144
LOG2E = 1.4426950408889634
LOW = -1e30
AXES = ("sp_0", "sp_1", "sp_2", "tp")
SP_TP = AXES
MESH = pl.DeviceIdType.MESH
f32 = jnp.float32
bf16 = jnp.bfloat16


def remote(src, dst, send, recv, device):
    return pltpu.make_async_remote_copy(
        src_ref=src, dst_ref=dst, send_sem=send, recv_sem=recv,
        device_id=device, device_id_type=MESH,
    )


def three(x):
    a = x.astype(bf16).astype(f32)
    r = x - a
    b = r.astype(bf16).astype(f32)
    return a, b, r - b


def iota(shape, dim):
    return lax.broadcasted_iota(jnp.int32, shape, dim)


def dot(a, b):
    return jnp.dot(a, b, preferred_element_type=f32)


def dot_t(a, b):
    return lax.dot_general(a, b, (((1,), (1,)), ((), ())), preferred_element_type=f32)


def block_rank(core, a, b):
    zz = a * (1 - core) + b * core
    yy = b * (1 - core) + a * core
    return zz * 16 + yy * 2 + core


def layer_kernel(
    tokens, w_q, w_kt, w_vt, w_gt, bias, w_o, out,
    x_all, wq_v, wk_v, wv_v, wg_v, bias_v, w_all, buf, sums_of, q_aug, q_far, q_near, peak, accum, table,
    att, heads,
    local, tok_send, tok_recv, one_send, one_recv, ta_send, ta_recv, tb_send, tb_recv,
    ts_send, ts_recv, right_send, right_recv, left_send, left_recv, sib_send, sib_recv,
    q_send, q_recv, w_send, w_recv, ws_send, ws_recv, att_send, att_recv,
):
    z, y, c, x = (lax.axis_index(a) for a in AXES)
    a0 = z * (1 - c) + y * c
    b0 = y * (1 - c) + z * c
    my_slot = c * 64 + a0 * 8 + b0
    rank = z * 16 + y * 2 + c
    across = [(z, y, c, lax.rem(x + k, 4)) for k in range(1, 4)]
    ring = [(lax.rem(z + k * c, 8), lax.rem(y + k * (1 - c), 8), c, x) for k in range(1, 8)]
    cross = [(lax.rem(z + k * (1 - c), 8), lax.rem(y + k * c, 8), c, x) for k in range(1, 8)]
    right, left = cross[0], cross[6]
    sibling = (z, y, 1 - c, x)
    mirrors = [(7 - z, y, 1 - c, g) for g in range(4)]
    mirror = (7 - z, y, 1 - c, x)
    far_rank = (7 - z) * 16 + y * 2 + 1 - c

    loads = [
        pltpu.make_async_copy(src, dst, local.at[i])
        for i, (src, dst) in enumerate((
            (tokens, x_all.at[x]), (w_kt, wk_v), (w_vt, wv_v), (w_gt, wg_v), (bias, bias_v),
            (w_q, wq_v), (w_o, w_all.at[x]),
        ))
    ]
    for load in loads:
        load.start()
    barrier = pltpu.get_barrier_semaphore()
    peers = [*mirrors, *cross, *ring, *across, sibling]
    for peer in peers:
        pl.semaphore_signal(barrier, inc=1, device_id=peer, device_id_type=MESH)
    loads[0].wait()
    pl.semaphore_wait(barrier, len(peers))

    def piece(owner, half):
        return x_all.at[owner, pl.ds(half * 32, 32)]

    def tok(i):
        half = (0, 1, 1, 0, 0, 1)[i]
        owner = (x, x, x, x, lax.rem(x + 3, 4), lax.rem(x + 1, 4))[i]
        ref = piece(owner, half)
        return remote(ref, ref, tok_send.at[i], tok_recv.at[i], across[(0, 0, 2, 2, 0, 2)[i]])

    for i in (0, 2, 1, 3):
        tok(i).start()

    for i in (0, 2):
        tok(i).wait_recv()
        tok(4 + i // 2).start()
    buf[128] = jnp.zeros((ROWS, BLOCK), bf16)
    lanes = iota((4 * HALF, 128), 1)
    selector = (
        (lanes < 12) & (lax.rem(lanes, 4) == iota((4 * HALF, 128), 0) // HALF)
    ).astype(f32).astype(bf16)
    q_aug[0, :, 128:256] = selector
    q_aug[1, :, 128:256] = selector
    peak[...] = jnp.full(peak.shape, LOW, f32)
    accum[...] = jnp.zeros(accum.shape, f32)
    for load in loads[1:]:
        load.wait()
    for i in (1, 3, 4, 5):
        tok(i).wait_recv()

    rows = x_all[...].reshape(BLOCK, x_all.shape[2])
    gates = dot_t(wg_v[...], rows).astype(bf16).astype(f32)
    spread = jnp.broadcast_to(bias_v[...], (4, 4))
    column = jnp.sum(jnp.where(iota((4, 4), 0) == iota((4, 4), 1), spread, 0.0), axis=1, keepdims=True)
    gates = jnp.concatenate([gates + column, jnp.zeros((4, BLOCK), f32)], axis=0)
    buf[my_slot, 0:HEAD, :] = dot_t(wk_v[...], rows).astype(bf16)
    buf[my_slot, HEAD:HALF, :] = dot_t(wv_v[...], rows).astype(bf16)
    small = jnp.exp(-jnp.abs(gates))
    series = small * (1.0 - small * (0.5 - small * (1 / 3 - small * (0.25 - small * 0.2))))
    logs = jnp.minimum(gates, 0.0) - jnp.where(small < 0.02, series, jnp.log(1.0 + small))
    tri = (iota((BLOCK, BLOCK), 0) <= iota((BLOCK, BLOCK), 1)).astype(f32).astype(bf16)
    pieces = jnp.concatenate([*three(logs), jnp.zeros((8, BLOCK), f32)], axis=0)
    sums = dot(pieces.astype(bf16), tri)
    decay = (sums[0:8] + sums[8:16] + sums[16:24]) * (-LOG2E)
    hi, mid, lo = three(decay)
    row = iota((8, BLOCK), 0)
    first = jnp.where(row < 4, hi, pltpu.roll(mid, 4, 0))
    second = jnp.where(row < 4, lo, 0.0)
    last = jnp.broadcast_to(decay[:, BLOCK - 1 : BLOCK], (8, 128))
    ends = jnp.where((iota((8, 128), 0) == iota((8, 128), 1)) & (iota((8, 128), 0) < 4), last, 0.0)
    sums_of[c, a0, b0] = jnp.sum(ends, axis=0, keepdims=True)
    buf[my_slot, HALF:ROWS, :] = jnp.concatenate([first, second], axis=0).astype(bf16)

    own_sum = sums_of.at[c, a0, b0]
    tas = [remote(own_sum, own_sum, ta_send.at[k], ta_recv.at[k], ring[k]) for k in range(7)]
    for k in range(7):
        tas[k].start()
    own = buf.at[my_slot]
    ones = [remote(own, own, one_send.at[k], one_recv.at[k], ring[k]) for k in range(7)]
    for k in (3, 2, 4, 1, 5, 0, 6):
        ones[k].start()

    queries = dot(rows, wq_v[...]).astype(bf16)
    q_far[...] = queries[HALF:]

    def expand(part, raw):
        scaled = raw.astype(f32) * (LOG2E * HEAD**-0.5)
        top = scaled.astype(bf16).astype(f32)
        rest = scaled - top
        for h in range(4):
            cols = slice(h * HEAD, (h + 1) * HEAD)
            both = jnp.concatenate([top[:, cols], rest[:, cols]], axis=1)
            q_aug[part, h * HALF : (h + 1) * HALF, 0:128] = both.astype(bf16)

    expand(0, queries[0:HALF])
    for i in range(6):
        tok(i).wait_send()
    q_copy = remote(q_far, q_near, q_send, q_recv, mirror)
    q_copy.start()
    half_rows = pl.ds(pl.multiple_of(c * 128, 128), 128)
    own_half = w_all.at[x, half_rows]
    w_copies = [remote(own_half, own_half, w_send.at[k], w_recv.at[k], across[k]) for k in range(3)]
    for k in (0, 2, 1):
        w_copies[k].start()

    for k in range(7):
        tas[k].wait()
    eight = sums_of.at[c, a0]
    tbs = [remote(eight, eight, tb_send.at[k], tb_recv.at[k], cross[k]) for k in range(7)]
    for k in range(7):
        tbs[k].start()

    def chunk(core, a, ch):
        return buf.at[pl.ds(core * 64 + a * 8 + ch * 4, 4)]

    def to_right(d, ch, i):
        ref = chunk(c, lax.rem(a0 - d + 8, 8), ch)
        return remote(ref, ref, right_send.at[i], right_recv.at[i], right)

    def to_left(d, ch, i):
        ref = chunk(c, lax.rem(a0 + d, 8), ch)
        return remote(ref, ref, left_send.at[i], left_recv.at[i], left)

    def to_sibling(a, ch, i):
        ref = chunk(c, a, ch)
        return remote(ref, ref, sib_send.at[i], sib_recv.at[i], sibling)

    for k in range(7):
        ones[k].wait()
    for ch in range(2):
        to_right(0, ch, ch).start()
        to_left(0, 1 - ch, ch).start()
    for ch in range(2):
        to_sibling(a0, ch, ch).start()

    for k in range(7):
        tbs[k].wait()
    core_sums = sums_of.at[c]
    share = remote(core_sums, core_sums, ts_send, ts_recv, sibling)
    share.start()
    q_copy.wait()
    expand(1, q_near[...])
    share.wait()

    def slot_rank(dim):
        s = iota((128, 128), dim)
        core = s // 64
        a = lax.rem(s // 8, 8)
        b = lax.rem(s, 8)
        return block_rank(core, a, b)

    before = (slot_rank(1) < slot_rank(0)).astype(f32).astype(bf16)
    all_sums = sums_of[...].reshape(128, 128)
    offset = None
    for piece in three(all_sums):
        part_of = dot(before, piece.astype(bf16))
        offset = part_of if offset is None else offset + part_of
    for h in range(4):
        table[h, 0:128] = jnp.broadcast_to(offset[:, h : h + 1], (128, 128))
        table[h, 128:136] = jnp.full((8, 128), LOW, f32)

    def tile(part, slots, masked):
        count = len(slots)
        keys = count * BLOCK

        def joined(lo, hi):
            return jnp.concatenate([buf[slot, lo:hi, :] for slot in slots], axis=1)

        k_t = joined(0, HEAD)
        right_side = jnp.concatenate(
            [k_t, k_t, joined(HALF, ROWS), jnp.zeros((112, keys), bf16)], axis=0
        )
        scores = dot(q_aug[part], right_side)
        allowed = None
        if masked:
            q_at = part * HALF + lax.rem(iota((4 * HALF, BLOCK), 0), HALF)
            allowed = iota((4 * HALF, BLOCK), 1) <= q_at
            scores = jnp.where(allowed, scores, LOW)
        shifts = []
        highest = None
        for u in range(count):
            shift = jnp.concatenate(
                [jnp.broadcast_to(table[h, pl.ds(slots[u], 1), :], (HALF, 128)) for h in range(4)],
                axis=0,
            )
            s = scores[:, u * BLOCK : (u + 1) * BLOCK]
            most = jnp.maximum(s[:, 0:128], s[:, 128:256]) + shift
            highest = most if highest is None else jnp.maximum(highest, most)
            shifts.append(shift)
        old = peak[part]
        new = jnp.maximum(old, jnp.max(highest, axis=1, keepdims=True))
        weights = []
        for u in range(count):
            base = new - shifts[u]
            for v in range(2):
                at = u * BLOCK + v * 128
                w = jnp.exp2(scores[:, at : at + 128] - base)
                if masked:
                    w = jnp.where(allowed[:, v * 128 : (v + 1) * 128], w, 0.0)
                weights.append(w.astype(bf16))
        v_t = jnp.concatenate(
            [joined(HEAD, HALF), jnp.ones((16, keys), bf16), jnp.zeros((48, keys), bf16)], axis=0
        )
        gained = dot_t(jnp.concatenate(weights, axis=1), v_t)
        accum[part] = accum[part] * jnp.exp2(old - new) + gained
        peak[part] = new

    def w_share(k):
        ref = w_all.at[lax.rem(x + 3 - k, 4), half_rows]
        return remote(ref, ref, ws_send.at[k], ws_recv.at[k], sibling)

    def arrival(i, side, core):
        d = (i + 2) // 2
        later = jnp.minimum(i + 1, 1)
        odd = lax.rem(i + 2, 2)
        ch = (odd * (1 - side) + (1 - odd) * side) * later + side * (1 - later)
        center = z * (1 - core) + y * core
        return lax.rem(center + 8 + d * (2 * side - 1), 8), ch

    owners = (rank, far_rank)
    diagonals = (
        my_slot,
        (1 - c) * 64 + ((7 - z) * c + y * (1 - c)) * 8 + y * c + (7 - z) * (1 - c),
    )

    def needed(n):
        starts = []
        numbers = ([], [])
        for i, core, live in ((n - 1, c, n <= 7), (n - 2, 1 - c, n >= 1)):
            at = jnp.maximum(jnp.minimum(i, 6), -1)
            for side in range(2):
                a, ch = arrival(at, side, core)
                starts.append(core * 64 + a * 8 + ch * 4)
                for part in range(2):
                    whole = sum(
                        (block_rank(core, a, ch * 4 + u) < owners[part]).astype(jnp.int32)
                        for u in range(4)
                    )
                    numbers[part].append(whole * live.astype(jnp.int32))
        return starts, numbers

    def pick(k, starts, number):
        first, second = number[0], number[0] + number[1]
        third = second + number[2]
        fourth = third + number[3]
        slot = jnp.where(k < third, starts[2] + k - second, starts[3] + k - third)
        slot = jnp.where(k < second, starts[1] + k - first, slot)
        slot = jnp.where(k < first, starts[0] + k, slot)
        return jnp.where(k < fourth, slot, 128)

    def to(owner):
        part = owner // 2
        device = mirrors[owner] if part else (z, y, c, owner)
        src = att.at[part, pl.ds((owner % 2) * 64, 64), :]
        return remote(src, heads.at[x], att_send.at[owner], att_recv.at[x], device)

    def finish(part):
        total_of = accum[part]
        result = total_of[:, 0:HEAD] / total_of[:, HEAD : HEAD + 1]
        for h in range(4):
            att[part, :, h * HEAD : (h + 1) * HEAD] = result[h * HALF : (h + 1) * HALF].astype(bf16)
        if part:
            to(2).start()
            to(3).start()
            return
        for owner in range(2):

            @pl.when(x != owner)
            def _(owner=owner):
                to(owner).start()

            @pl.when(x == owner)
            def _(owner=owner):
                heads[owner] = att[0, owner * 64 : (owner + 1) * 64, :]

    def round_of(n, kept):
        i = n - 1

        @pl.when((n >= 1) & (n <= 7))
        def _():
            d = (i + 2) // 2
            a_r, ch_r = arrival(i, 0, c)
            a_l, ch_l = arrival(i, 1, c)
            to_right(0, 0, i).wait_recv()

            @pl.when(i <= 4)
            def _():
                to_right(d, ch_r, i + 2).start()

            to_left(0, 0, i).wait_recv()

            @pl.when(i <= 4)
            def _():
                to_left(d, ch_l, i + 2).start()

            to_sibling(a_r, ch_r, 2 + 2 * i).start()
            to_sibling(a_l, ch_l, 3 + 2 * i).start()

        @pl.when(n >= 1)
        def _():
            to_sibling(a0, 0, 2 * i).wait_recv()
            to_sibling(a0, 0, 2 * i + 1).wait_recv()

        @pl.when(n == 6)
        def _():
            for k in range(3):
                w_copies[k].wait()
                w_share(k).start()

        @pl.when((n == 0) | (n == 7))
        def _():
            part = n // 7
            tile(part, [diagonals[0] * (1 - part) + diagonals[1] * part], True)

        starts, numbers = needed(n)
        fresh = [sum(numbers[part]) for part in range(2)]
        tiles = [(kept[part][0] + fresh[part] + 7 * (n // 8)) // 8 for part in range(2)]

        def one_tile(k, carry):
            part = (k < tiles[1]).astype(jnp.int32)
            first = (k - (1 - part) * tiles[1]) * 8
            number = [numbers[0][q] * (1 - part) + numbers[1][q] * part for q in range(4)]
            held = [kept[0][q] * (1 - part) + kept[1][q] * part for q in range(8)]
            slots = []
            for u in range(8):
                slot = pick(first + u - held[0], starts, number)
                if u < 7:
                    slot = jnp.where(first + u < held[0], held[1 + u], slot)
                slots.append(slot)
            tile(part, slots, False)

            @pl.when((n == 8) & (k == tiles[1] - 1))
            def _():
                finish(1)

            return carry

        @pl.when((n == 8) & (tiles[1] == 0))
        def _():
            finish(1)

        lax.fori_loop(0, tiles[0] + tiles[1], one_tile, 0)
        after = []
        for part in range(2):
            first = tiles[part] * 8
            rest = [jnp.maximum(kept[part][0] + fresh[part] - first, 0)]
            for u in range(7):
                slot = pick(first + u - kept[part][0], starts, numbers[part])
                rest.append(jnp.where(first + u < kept[part][0], kept[part][1 + u], slot))
            after.append(tuple(rest))
        return tuple(after)

    nothing = tuple(jnp.int32(0) for _ in range(8))
    lax.fori_loop(0, 9, round_of, (nothing, nothing))

    finish(0)

    for k in range(3):
        w_share(k).wait()
    def drain(i, carry):
        to_sibling(a0, 0, i).wait_send()
        return carry

    lax.fori_loop(0, 16, drain, 0)

    def drain_ring(i, carry):
        to_right(0, 0, i).wait_send()
        to_left(0, 0, i).wait_send()
        return carry

    lax.fori_loop(0, 7, drain_ring, 0)

    for g in range(4):

        @pl.when((x >= 2) | (x != g))
        def _(g=g):
            src = att.at[0, pl.ds(0, 64), :]
            remote(src, heads.at[g], att_send.at[0], att_recv.at[g], mirrors[0]).wait_recv()

    for col in range(0, out.shape[1], 512):
        total = None
        for g in range(4):
            part = dot(heads[g], w_all[g, :, col : col + 512]).astype(bf16).astype(f32)
            total = part if total is None else total + part
        out[:, col : col + 512] = total.astype(bf16)

    for owner in range(4):
        if owner < 2:

            @pl.when(x != owner)
            def _(owner=owner):
                to(owner).wait_send()
        else:
            to(owner).wait_send()


def shards(tokens, w_query, w_key, w_value, w_gate, gate_bias, w_output):
    d = tokens.shape[1]
    hbm = pl.BlockSpec(memory_space=pltpu.HBM)
    dma = pltpu.SemaphoreType.DMA
    vmem = pltpu.VMEM
    return pl.pallas_call(
        layer_kernel,
        name="layer",
        out_shape=jax.ShapeDtypeStruct(tokens.shape, bf16),
        in_specs=[hbm] * 7,
        out_specs=pl.BlockSpec(memory_space=pltpu.VMEM),
        scratch_shapes=[
            vmem((4, *tokens.shape), bf16),
            vmem(w_query.shape, bf16),
            vmem((HEAD, d), bf16),
            vmem((HEAD, d), bf16),
            vmem((4, d), bf16),
            vmem((1, 4), f32),
            vmem((4, *w_output.shape), bf16),
            vmem((129, ROWS, BLOCK), bf16),
            vmem((2, 8, 8, 1, 128), f32),
            vmem((2, 4 * HALF, 256), bf16),
            vmem((HALF, 4 * HEAD), bf16),
            vmem((HALF, 4 * HEAD), bf16),
            vmem((2, 4 * HALF, 128), f32),
            vmem((2, 4 * HALF, 128), f32),
            vmem((4, 136, 128), f32),
            vmem((2, HALF, 4 * HEAD), bf16),
            vmem((4, 64, 4 * HEAD), bf16),
            dma((7,)),
            dma((6,)), dma((6,)),
            dma((7,)), dma((7,)),
            dma((7,)), dma((7,)),
            dma((7,)), dma((7,)),
            dma, dma,
            dma((7,)), dma((7,)),
            dma((7,)), dma((7,)),
            dma((16,)), dma((16,)),
            dma, dma,
            dma((3,)), dma((3,)),
            dma((3,)), dma((3,)),
            dma((4,)), dma((4,)),
        ],
        compiler_params=pltpu.CompilerParams(
            collective_id=0, has_side_effects=True, vmem_limit_bytes=56 * 2**20
        ),
    )(tokens, w_query, w_key.T, w_value.T, w_gate.T, gate_bias.reshape(1, -1), w_output)


def solution(mesh):
    finer = Mesh(mesh.devices.reshape(8, 8, 2, mesh.shape["tp"]), AXES)
    placed = (
        P(SP_TP, None),
        P(None, "tp"),
        P(None, "tp"),
        P(None, "tp"),
        P(None, "tp"),
        P("tp"),
        P("tp", None),
    )
    return jax.shard_map(
        shards, mesh=finer, in_specs=placed, out_specs=P(SP_TP, None), check_vma=False
    )
```
